128 devices in a mesh: ep: 128 (over z, y, x, core).
Axes of the slice: x: 4, y: 4, z: 4, core: 2. Of those that a mesh axis runs over, the one named last changes fastest.
Arguments:
- tokens: bfloat16 [2304, 2048], P('ep'), may hold values from -6 to 6
- attn_norm_gain: float32 [2048], replicated, may hold values from 0.1 to 1.9
- w_query: bfloat16 [2048, 512], replicated, may hold values from -0.125 to 0.125
- w_key: bfloat16 [2048, 128], replicated, may hold values from -0.125 to 0.125
- w_value: bfloat16 [2048, 128], replicated, may hold values from -0.125 to 0.125
- w_forget: bfloat16 [2048, 8], replicated, may hold values from -0.125 to 0.125
- forget_bias: float32 [8], replicated, may hold values from 0.5 to 4
- w_attn_out: bfloat16 [512, 2048], replicated, may hold values from -0.25 to 0.25
- cache_keys: bfloat16 [2304, 1024, 128], P('ep'), may hold values from -72 to 72
- cache_values: bfloat16 [2304, 1024, 128], P('ep'), may hold values from -6 to 6
- cache_logcum: float32 [2304, 8, 1024], P('ep'), as said below
- cache_lengths: int32 [2304], P('ep'), may hold values from 128 to 1024
- expert_norm_gain: float32 [2048], replicated, may hold values from 0.4 to 40
- expert_ids: int32 [2304, 6], P('ep'), may hold values from 0 to 127, all different within a row; in each aligned block of 18 rows (0 to 17, 18 to 35, ...) at most 2 rows name the same one
- expert_weights: float32 [2304, 6], P('ep'), may hold values from 0.1 to 1
- w_expert_gate: bfloat16 [128, 2048, 512], P('ep'), may hold values from -0.125 to 0.125
- w_expert_up: bfloat16 [128, 2048, 512], P('ep'), may hold values from -0.125 to 0.125
- w_expert_down: bfloat16 [128, 512, 2048], P('ep'), may hold values from -0.25 to 0.25
- w_dense_gate: bfloat16 [2048, 4096], P(None, 'ep'), may hold values from -0.125 to 0.125
- w_dense_up: bfloat16 [2048, 4096], P(None, 'ep'), may hold values from -2 to 2
- w_dense_down: bfloat16 [4096, 2048], P('ep'), may hold values from -0.09375 to 0.09375
- dense_norm_gain: float32 [4096], replicated, may hold values from 0.1 to 1.9
- branch_gate: float32 [2048], replicated, may hold values from -0.125 to 0.125
Outputs:
- result: bfloat16 [2304, 2048], P('ep')
The draws below stay inside these ranges and needn't reach their ends.
Inputs may be any that keep to these rules, and one draw needn't show every extreme that they name: `cache_logcum`: along the positions of each sequence and head the values never rise. `expert_ids`: each row names 6 different experts; among the rows of one device no expert is named by more than 2 rows, and in every draw some device names some expert exactly 2 times.
All inputs are finite; a program needn't handle non-finite values.
Results may differ from the reference program's by a relative error of at most 0.012.
The reference program's roundings to bfloat16 on the way count: a program that leaves them out, or rounds other values in their place, can miss the bound.
Values may be sent and summed in bfloat16 or wider, within the bound.
No kernel may reach another device: no remote copies, remote signals or barrier semaphores. Data moves between devices by JAX's collectives and lax.ppermute only.
A program may use at most 128 MiB of HBM per device.

```python
import math
import jax
import jax.numpy as jnp
import numpy as np
from jax import lax

D = 2048
HEADS = 8
KV_HEADS = 2
HEAD_DIM = 64
EXPERT_FF = 512
DENSE_FF = 4096
TOPK = 6
SEQ_DEV = 18
CACHE_POSITIONS = 1024
SEQS = 2304
EXPERTS = 128
CAP = 2
N_EP = 128


def draw_cache_keys(key, part):
    tensor_extent = (SEQS, CACHE_POSITIONS, KV_HEADS * HEAD_DIM)
    base = jnp.clip(jax.random.normal(jax.random.fold_in(key, 11), tensor_extent, jnp.float32), -6.0, 6.0)
    values = base
    return jnp.clip(values, -72.0, 72.0).astype(jnp.bfloat16)


def draw_cache_logcum(key, part):
    tensor_extent = (SEQS, HEADS, CACHE_POSITIONS)
    order = jax.random.permutation(jax.random.fold_in(key, 21), HEADS)
    gradual_decay = (order < HEADS // 2)[None, :, None]
    chain_total = jax.random.uniform(jax.random.fold_in(key, 22), (SEQS, HEADS, 1), jnp.float32, 0.3, 1.5)
    fast_span = jax.random.uniform(jax.random.fold_in(key, 23), (SEQS, HEADS, 1), jnp.float32, 30.0, 100.0)
    decay_speed = jnp.where(gradual_decay, chain_total / CACHE_POSITIONS, 1.0 / fast_span)
    sequence_multiplier = jnp.exp(jax.random.uniform(jax.random.fold_in(key, 24), (SEQS, 1, 1), jnp.float32, -0.7, 0.7))
    coarse_estimate = jnp.exp(jax.random.uniform(jax.random.fold_in(key, 25), tensor_extent, jnp.float32, -0.7, 0.7))
    spike_position = jax.random.uniform(jax.random.fold_in(key, 26), tensor_extent, jnp.float32) < 3.0 / CACHE_POSITIONS
    spike_amount = -jnp.log(jax.random.uniform(jax.random.fold_in(key, 27), tensor_extent, jnp.float32, 0.5, 0.8))
    step_numbers = decay_speed * sequence_multiplier * coarse_estimate + jnp.where(spike_position & gradual_decay, spike_amount, 0.0)
    return -jnp.cumsum(step_numbers, axis=2)


def draw_expert_norm_gain(key, part):
    base = 1.0 + 0.18 * jnp.clip(jax.random.normal(jax.random.fold_in(key, 31), (D,), jnp.float32), -3.0, 3.0)
    return base


def draw_w_dense_up(key, part):
    normal_part = jnp.clip(jax.random.normal(jax.random.fold_in(key, 41), (D, DENSE_FF), jnp.float32), -6.0, 6.0)
    column = jnp.arange(DENSE_FF, dtype=jnp.float32)[None, :] / DENSE_FF
    scale = 3.0 ** column * jnp.exp(jax.random.uniform(jax.random.fold_in(key, 43), (1, DENSE_FF), jnp.float32, -0.3, 0.3))
    return jnp.clip(normal_part * D ** (-0.5) * scale, -2.0, 2.0).astype(jnp.bfloat16)


def with_ends(drawn, key, smallest, largest):
    shape = drawn.shape
    spot = [jax.random.randint(jax.random.fold_in(key, axis), (), 0, shape[axis]) for axis in range(len(shape))]
    drawn = drawn.at[tuple(spot)].set(smallest)
    longest = shape.index(max(shape))
    spot[longest] = (spot[longest] + 1) % shape[longest]
    return drawn.at[tuple(spot)].set(largest)


def steps_of(key, extent, cuts, least, top_value):
    factor_of = 1.0
    for axis_at, parts in cuts:
        steps = jax.random.uniform(jax.random.fold_in(jax.random.fold_in(key, 6), axis_at), (parts,), jnp.float32, least / len(cuts), top_value / len(cuts))
        factor_of = factor_of * jnp.repeat(jnp.exp(steps), extent[axis_at] // parts).reshape((-1,) + (1,) * (len(extent) - 1 - axis_at))
    return factor_of


def deal_out(rng, own, number, rows, number_of, top, most, lean):
    sequence = jax.random.permutation(rng, number_of)
    crowded, usual = shares(number_of, rows * top, most, lean, True), shares(number_of, rows * top, most, lean, False)
    places = jnp.arange(number_of)

    def named(tallies, rotation):
        used = int((tallies > 0).sum())
        fixed = max(1, used // 4)
        shifted = fixed + (places - fixed + rotation * (used - fixed)) % max(1, number_of - fixed)
        return jnp.zeros((number_of,), jnp.int32).at[sequence[jnp.where(places < fixed, places, shifted)]].set(jnp.asarray(tallies, jnp.int32))

    tallies = jnp.where(number % 4 == 0, named(crowded, number // 4), named(usual, number - number // 4 - 1))
    mixed = jax.random.permutation(jax.random.fold_in(own, 3), number_of)
    giver, receiver = mixed[0:number_of // 2 * 2:2], mixed[1:number_of // 2 * 2:2]
    margin = jnp.minimum(tallies[giver] - 1, most - tallies[receiver]) // 2
    margin = jnp.where((giver == sequence[0]) | (receiver == sequence[0]) | (tallies[receiver] == 0), 0, jnp.maximum(margin, 0))
    shifted = jax.random.randint(jax.random.fold_in(own, 4), (number_of // 2,), 0, 1 << 20) % (margin + 1)
    tallies = tallies.at[giver].add(-shifted).at[receiver].add(shifted)
    labels = jnp.searchsorted(jnp.cumsum(tallies), jnp.arange(rows * top), side="right").astype(jnp.int32)
    listing = labels.reshape(top, rows).T
    listing = listing[jax.random.permutation(jax.random.fold_in(own, 1), rows)]
    rotation = jax.random.randint(jax.random.fold_in(own, 2), (rows, 1), 0, top)
    return jnp.take_along_axis(listing, (jnp.arange(top)[None, :] + rotation) % top, axis=1)


def shares(number_of, total, limit, skew, full):
    loads = [(1 << 20) // math.isqrt(standing ** skew) + 1 for standing in range(1, number_of + 1)]
    largest = limit if full else min(limit, max(-(-total // number_of), total * loads[0] // sum(loads)))
    least = 1 if total - largest >= number_of - 1 else 0
    given, spare = [largest] + [least] * (number_of - 1), total - largest - least * (number_of - 1)
    while spare > 0:
        candidates = [i for i in range(1, number_of) if given[i] < largest] or [i for i in range(1, number_of) if given[i] < limit]
        whole, budget = sum([loads[i] for i in candidates]), spare
        for i in candidates:
            extra = min(limit - given[i], max(1, budget * loads[i] // whole), spare)
            given[i] = given[i] + extra
            spare = spare - extra
    return np.array(given)


def centred(rng, extent, deviation, bound, shards=(), held_as=jnp.bfloat16):
    values = deviation * jax.random.normal(rng, extent, jnp.float32)
    if shards:
        values = values * steps_of(rng, extent, shards, -0.22, 0.18)
    return jnp.clip(values, -bound, bound).astype(held_as)


def setup_inputs(seed: int = 0) -> dict:
    splits = jax.random.split(jax.random.key(seed), 24)
    tokens = centred(splits[0], (SEQS, D), 1.0, 6.0, ((0, 128),))
    attn_norm_gain = jnp.clip(1.0 + 0.18 * jax.random.normal(splits[1], (D,), jnp.float32), 0.1, 1.9)
    w_query = centred(splits[2], (D, HEADS * HEAD_DIM), D ** -0.5, 0.125)
    w_key = centred(splits[3], (D, KV_HEADS * HEAD_DIM), D ** -0.5, 0.125)
    w_value = centred(splits[4], (D, KV_HEADS * HEAD_DIM), D ** -0.5, 0.125)
    w_forget = centred(splits[5], (D, HEADS), D ** -0.5, 0.125)
    forget_bias = jnp.clip(jax.random.uniform(splits[6], (HEADS,), jnp.float32, 0.5, 4.0), 0.5, 4.0)
    w_attn_out = centred(splits[7], (HEADS * HEAD_DIM, D), (HEADS * HEAD_DIM) ** -0.5, 0.25)
    cache_keys = draw_cache_keys(jax.random.fold_in(splits[23], 71), 0)
    cache_values = centred(splits[9], (SEQS, CACHE_POSITIONS, KV_HEADS * HEAD_DIM), 1.0, 6.0, ((0, 128),))
    cache_logcum = draw_cache_logcum(jax.random.fold_in(splits[23], 71), 0)
    cache_lengths = with_ends(jax.random.randint(splits[11], (SEQS,), CACHE_POSITIONS // 8, CACHE_POSITIONS + 1), jax.random.fold_in(splits[11], 1), CACHE_POSITIONS // 8, CACHE_POSITIONS).astype(jnp.int32)
    expert_norm_gain = draw_expert_norm_gain(jax.random.fold_in(splits[23], 71), 0)
    expert_ids_keys = jax.random.split(jax.random.fold_in(splits[13], 1), SEQS // SEQ_DEV)
    expert_ids_turns = jax.random.permutation(jax.random.fold_in(splits[13], 3), SEQS // SEQ_DEV)
    expert_ids = jax.vmap(lambda own, number: deal_out(jax.random.fold_in(splits[13], 2), own, number, SEQ_DEV, EXPERTS, TOPK, CAP, 2))(expert_ids_keys, expert_ids_turns).reshape((SEQS, TOPK))
    expert_weights = jnp.clip(jnp.exp(math.log(1.0) - 2.3025851 * jax.random.uniform(splits[14], (SEQS, TOPK), jnp.float32) ** steps_of(splits[14], (SEQS, TOPK), ((0, 128),), -0.2, 0.2)), 0.1, 1.0)
    w_expert_gate = centred(splits[15], (EXPERTS, D, EXPERT_FF), D ** -0.5, 0.125, ((0, 128),))
    w_expert_up = centred(splits[16], (EXPERTS, D, EXPERT_FF), D ** -0.5, 0.125, ((0, 128),))
    w_expert_down = centred(splits[17], (EXPERTS, EXPERT_FF, D), EXPERT_FF ** -0.5, 0.25, ((0, 128),))
    w_dense_gate = centred(splits[18], (D, DENSE_FF), D ** -0.5, 0.125, ((1, 128),))
    w_dense_up = draw_w_dense_up(jax.random.fold_in(splits[23], 71), 0)
    w_dense_down = centred(splits[20], (DENSE_FF, D), DENSE_FF ** -0.5, 0.09375, ((0, 128),))
    dense_norm_gain = jnp.clip(1.0 + 0.18 * jax.random.normal(splits[21], (DENSE_FF,), jnp.float32), 0.1, 1.9)
    branch_gate = centred(splits[22], (D,), D ** -0.5, 0.125, (), jnp.float32)
    return dict(tokens=tokens, attn_norm_gain=attn_norm_gain, w_query=w_query, w_key=w_key, w_value=w_value, w_forget=w_forget, forget_bias=forget_bias, w_attn_out=w_attn_out, cache_keys=cache_keys, cache_values=cache_values, cache_logcum=cache_logcum, cache_lengths=cache_lengths, expert_norm_gain=expert_norm_gain, expert_ids=expert_ids, expert_weights=expert_weights, w_expert_gate=w_expert_gate, w_expert_up=w_expert_up, w_expert_down=w_expert_down, w_dense_gate=w_dense_gate, w_dense_up=w_dense_up, w_dense_down=w_dense_down, dense_norm_gain=dense_norm_gain, branch_gate=branch_gate)


EPS = 1e-06
LIMIT = 7.0
ALPHA = 1.702

def normalize(values, gain):
    return values * lax.rsqrt(lax.optimization_barrier(jnp.mean(values * values, axis=-1, keepdims=True)) + EPS) * gain

def stored(values):
    return lax.optimization_barrier(values.astype(jnp.bfloat16))

def attend(query, key_new, value_new, log_forget, cache_keys, cache_values, cache_logcum, cache_lengths):
    seqs, length = (cache_keys.shape[0], cache_keys.shape[1])
    group = HEADS // KV_HEADS
    scale = HEAD_DIM ** (-0.5)
    heads_q = query.astype(jnp.float32).reshape(seqs, KV_HEADS, group, HEAD_DIM)
    keys = cache_keys.astype(jnp.float32).reshape(seqs, length, KV_HEADS, HEAD_DIM)
    values = cache_values.astype(jnp.float32).reshape(seqs, length, KV_HEADS, HEAD_DIM)
    own_key = key_new.astype(jnp.float32).reshape(seqs, KV_HEADS, HEAD_DIM)
    own_value = value_new.astype(jnp.float32).reshape(seqs, KV_HEADS, 1, HEAD_DIM)
    last_index = jnp.broadcast_to((cache_lengths - 1)[:, None, None], (seqs, HEADS, 1)).astype(jnp.int32)
    carried = jnp.take_along_axis(cache_logcum, last_index, axis=2)[:, :, 0] + log_forget
    offset = (carried[:, :, None] - cache_logcum).reshape(seqs, KV_HEADS, group, length)
    scores = jnp.einsum('skgd,slkd->skgl', heads_q, keys) * scale + offset
    live = jnp.arange(length, dtype=jnp.int32)[None, :] < cache_lengths[:, None]
    scores = jnp.where(live[:, None, None, :], scores, -jnp.inf)
    own = jnp.einsum('skgd,skd->skg', heads_q, own_key) * scale
    top = jnp.maximum(lax.optimization_barrier(jnp.max(scores, axis=-1)), own)
    expo = jnp.exp(scores - top[..., None])
    own_expo = jnp.exp(own - top)
    total = lax.optimization_barrier(jnp.sum(expo, axis=-1)) + own_expo
    weights = stored(expo / total[..., None]).astype(jnp.float32)
    own_weight = stored(own_expo / total).astype(jnp.float32)
    out = jnp.einsum('skgl,slkd->skgd', weights, values) + own_weight[..., None] * own_value
    return out.reshape(seqs, HEADS * HEAD_DIM).astype(jnp.bfloat16)

def expert_unit(rows, gate_w, up_w, down_w):
    gate = jnp.minimum(jnp.dot(rows, gate_w, preferred_element_type=jnp.float32), LIMIT)
    up = jnp.clip(jnp.dot(rows, up_w, preferred_element_type=jnp.float32), -LIMIT, LIMIT)
    act = ((up + 1.0) * gate * jax.nn.sigmoid(gate * ALPHA)).astype(jnp.bfloat16)
    return jnp.dot(act, down_w, preferred_element_type=jnp.float32).astype(jnp.bfloat16)

def reference(tokens, attn_norm_gain, w_query, w_key, w_value, w_forget, forget_bias, w_attn_out, cache_keys, cache_values, cache_logcum, cache_lengths, expert_norm_gain, expert_ids, expert_weights, w_expert_gate, w_expert_up, w_expert_down, w_dense_gate, w_dense_up, w_dense_down, dense_norm_gain, branch_gate):
    seqs = tokens.shape[0]
    normed = normalize(tokens.astype(jnp.float32), attn_norm_gain).astype(jnp.bfloat16)
    query = jnp.dot(normed, w_query, preferred_element_type=jnp.float32).astype(jnp.bfloat16)
    key_new = jnp.dot(normed, w_key, preferred_element_type=jnp.float32).astype(jnp.bfloat16)
    value_new = jnp.dot(normed, w_value, preferred_element_type=jnp.float32).astype(jnp.bfloat16)
    log_forget = jax.nn.log_sigmoid(jnp.dot(normed, w_forget, preferred_element_type=jnp.float32) + forget_bias)

    def one_block(index):
        start = index * SEQ_DEV

        def pick(array):
            return lax.dynamic_slice_in_dim(array, start, SEQ_DEV, 0)
        return attend(pick(query), pick(key_new), pick(value_new), pick(log_forget), pick(cache_keys), pick(cache_values), pick(cache_logcum), pick(cache_lengths))
    attended = lax.map(one_block, jnp.arange(N_EP, dtype=jnp.int32)).reshape(seqs, HEADS * HEAD_DIM)
    mixed = stored(tokens.astype(jnp.float32) + jnp.dot(attended, w_attn_out, preferred_element_type=jnp.float32))
    routed_in = normalize(mixed.astype(jnp.float32), expert_norm_gain).astype(jnp.bfloat16)
    flat_ids = expert_ids.reshape(-1)
    rows_all = flat_ids.shape[0]
    room = N_EP * CAP

    def run_expert(outputs, expert):
        chosen = flat_ids == expert
        order = jnp.cumsum(chosen.astype(jnp.int32)) - 1
        where_to = jnp.where(chosen, order, room).astype(jnp.int32)
        source = jnp.zeros((room,), jnp.int32).at[where_to].set(jnp.arange(rows_all, dtype=jnp.int32), mode='drop')
        picked = jnp.take(routed_in, source // TOPK, axis=0)
        answer = expert_unit(picked, w_expert_gate[expert], w_expert_up[expert], w_expert_down[expert])
        filled = jnp.arange(room, dtype=jnp.int32) < jnp.sum(chosen.astype(jnp.int32))
        target = jnp.where(filled, source, rows_all).astype(jnp.int32)
        return (outputs.at[target].set(answer, mode='drop'), None)
    outputs = lax.scan(run_expert, jnp.zeros((rows_all, D), jnp.bfloat16), jnp.arange(EXPERTS, dtype=jnp.int32))[0]
    routed = lax.optimization_barrier(jnp.sum(expert_weights[:, :, None] * outputs.astype(jnp.float32).reshape(seqs, TOPK, D), axis=1))
    gate_dense = jnp.dot(routed_in, w_dense_gate, preferred_element_type=jnp.float32)
    up_dense = jnp.dot(routed_in, w_dense_up, preferred_element_type=jnp.float32)
    units = stored(jax.nn.silu(gate_dense) * up_dense).astype(jnp.float32)
    unit_scale = lax.rsqrt(lax.optimization_barrier(jnp.mean(units * units, axis=1, keepdims=True)) + EPS)
    hidden = (units * unit_scale * dense_norm_gain).astype(jnp.bfloat16)
    dense = jnp.dot(hidden, w_dense_down, preferred_element_type=jnp.float32)
    branch_scale = jax.nn.sigmoid(lax.optimization_barrier(jnp.sum(routed_in.astype(jnp.float32) * branch_gate, axis=1, keepdims=True)))
    return (mixed.astype(jnp.float32) + routed + branch_scale * dense).astype(jnp.bfloat16)
```

```python
import jax
import jax.numpy as jnp
from jax import lax
from jax.experimental import pallas as pl
from jax.experimental.pallas import tpu as pltpu
from jax.sharding import PartitionSpec as P

HEADS = 8
KV_HEADS = 2
HEAD_DIM = 64
TOPK = 6
EPS = 1e-06
LIMIT = 7.0
ALPHA = 1.702
CAP = 2
PLANE = 32
CORES = 2
PARTS = 8
DENSE_FF = 4096
F32 = jnp.float32
BF16 = jnp.bfloat16
VMEM = pl.BlockSpec(memory_space=pltpu.VMEM)
ANY = pl.BlockSpec(memory_space=pl.ANY)
NT = (((1,), (1,)), ((), ()))
TN = (((0,), (0,)), ((), ()))


def dot(a, b):
    return jnp.dot(a, b, preferred_element_type=F32)


def slot_masks(slots, seqs):
    slot = lax.broadcasted_iota(jnp.int32, (slots, seqs), 0)
    token = lax.broadcasted_iota(jnp.int32, (slots, seqs), 1)
    device = slot // CAP
    part = (device // PLANE) * CORES + device % CORES
    dense = token == part + PARTS * (slot % CAP)
    extra = token == part + PARTS * CAP
    return slot, device, dense, extra


def fill_outgoing(routed_in, ids_ref, eweights_ref, place_ref, outgoing_ref):
    seqs, width = routed_in.shape
    half = width // CAP
    slots = outgoing_ref.shape[0] * CAP
    slot, device, dense, extra = slot_masks(slots, seqs)
    member = jnp.zeros((slots, seqs), F32)
    share = jnp.zeros((slots, seqs), F32)
    for k in range(TOPK):
        hit = ids_ref[k:k + 1, :] == device
        member = member + jnp.where(hit, 1.0, 0.0)
        share = share + jnp.where(hit, eweights_ref[k:k + 1, :], 0.0)
    earlier = lax.broadcasted_iota(jnp.int32, (seqs, seqs), 0)
    later = lax.broadcasted_iota(jnp.int32, (seqs, seqs), 1)
    before = jnp.where(earlier < later, 1.0, 0.0).astype(BF16)
    prior = dot(member.astype(BF16), before)
    here = prior == (slot % CAP).astype(F32)
    place_ref[...] = jnp.where(here, share, 0.0)
    routes = jnp.where(here, member, 0.0).astype(BF16)
    extra = jnp.where(extra, 1.0, 0.0).astype(BF16)
    even = lax.broadcasted_iota(jnp.int32, (slots, half), 0) % CAP == 0
    third = jnp.where(even, dot(extra, routed_in[:, :half]), dot(extra, routed_in[:, half:]))
    devices = slots // CAP
    outgoing_ref[:, :, :width] = dot(routes, routed_in).astype(BF16).reshape(devices, CAP, width)
    outgoing_ref[:, :, width:2 * width] = dot(
        jnp.where(dense, 1.0, 0.0).astype(BF16), routed_in).astype(BF16).reshape(devices, CAP, width)
    outgoing_ref[:, :, 2 * width:] = third.astype(BF16).reshape(devices, CAP, half)


def mixer_body(
    tokens_ref, again_ref, wq_hbm, wk_hbm, wv_hbm, wf_ref, fbias_ref, wo_hbm,
    keys_hbm, values_hbm, logcum_hbm, lengths_ref, egain_ref, bgate_ref, ids_ref, eweights_ref,
    mixed_ref, branch_ref, place_ref, outgoing_ref,
    wq, wk, wv, wo, kbuf, vbuf, cbuf, sems,
):
    seqs, width = tokens_ref.shape
    length = kbuf.shape[1]
    rows = seqs * HEADS
    copies = [
        pltpu.make_async_copy(wq_hbm, wq, sems.at[0]),
        pltpu.make_async_copy(wk_hbm, wk, sems.at[1]),
        pltpu.make_async_copy(wv_hbm, wv, sems.at[2]),
        pltpu.make_async_copy(keys_hbm, kbuf, sems.at[3]),
        pltpu.make_async_copy(logcum_hbm, cbuf, sems.at[4]),
        pltpu.make_async_copy(values_hbm, vbuf, sems.at[5]),
        pltpu.make_async_copy(wo_hbm, wo, sems.at[6]),
    ]
    for copy in copies:
        copy.start()
    x = tokens_ref[...].astype(F32)
    scale = lax.rsqrt(jnp.mean(x * x, axis=1, keepdims=True) + EPS)
    normed = (x * scale * again_ref[...]).astype(BF16)
    forget = lax.dot_general(normed, wf_ref[...], NT, preferred_element_type=F32) + fbias_ref[...]
    log_forget = jax.nn.log_sigmoid(forget)
    row = lax.broadcasted_iota(jnp.int32, (rows, seqs), 0)
    col = lax.broadcasted_iota(jnp.int32, (rows, seqs), 1)
    spread_mask = (row // HEADS) == col
    spread = jnp.where(spread_mask, 1.0, 0.0).astype(BF16)
    live_len = jnp.sum(jnp.where(spread_mask, lengths_ref[...], 0), axis=1, keepdims=True)
    head8 = lax.broadcasted_iota(jnp.int32, (rows, HEADS), 0) % HEADS
    lane8 = lax.broadcasted_iota(jnp.int32, (rows, HEADS), 1)
    lf_rows = lax.dot_general(
        jnp.where(spread_mask, 1.0, 0.0), log_forget, (((1,), (0,)), ((), ())),
        precision=lax.Precision.HIGHEST, preferred_element_type=F32)
    lf_rows = jnp.sum(jnp.where(head8 == lane8, lf_rows, 0.0), axis=1, keepdims=True)

    for i in range(3):
        copies[i].wait()
    query = dot(normed, wq[...]).astype(BF16)
    key_new = dot(normed, wk[...]).astype(BF16)
    value_new = dot(normed, wv[...]).astype(BF16)
    q_rows = dot(spread, query)
    key_rows = dot(spread, key_new)
    value_rows = dot(spread, value_new)
    head = lax.broadcasted_iota(jnp.int32, (rows, 128), 0) % HEADS
    lane = lax.broadcasted_iota(jnp.int32, (rows, 128), 1)
    half = lane // HEAD_DIM
    kv_half = head // (HEADS // KV_HEADS)
    q_sel = jnp.zeros((rows, 128), F32)
    for b in range(HEADS // 2):
        block = q_rows[:, 128 * b:128 * b + 128]
        turned = pltpu.roll(block, HEAD_DIM, 1)
        q_sel = jnp.where(head // 2 == b, jnp.where(head % 2 == kv_half, block, turned), q_sel)
    q_sel = jnp.where(half == kv_half, q_sel, 0.0)
    own = jnp.sum(q_sel * key_rows, axis=1, keepdims=True) * (HEAD_DIM ** -0.5)
    q_bf = q_sel.astype(BF16)
    seq_row = lax.broadcasted_iota(jnp.int32, (rows, 128), 0) // HEADS
    blocks = [jnp.where(seq_row == s, q_sel, 0.0).astype(BF16) for s in range(seqs)]
    q_block = jnp.concatenate(blocks, axis=1)

    copies[3].wait()
    k_all = jnp.concatenate([kbuf[s] for s in range(seqs)], axis=1)
    scores_t = lax.dot_general(k_all, q_block, NT, preferred_element_type=F32)
    scores = jnp.transpose(scores_t)
    copies[4].wait()
    logcum = cbuf[...].reshape(rows, length)
    place = lax.broadcasted_iota(jnp.int32, (rows, length), 1)
    last = jnp.sum(jnp.where(place == live_len - 1, logcum, 0.0), axis=1, keepdims=True)
    carried = last + lf_rows
    scores = scores * (HEAD_DIM ** -0.5) + (carried - logcum)
    scores = jnp.where(place < live_len, scores, -jnp.inf)
    top = jnp.maximum(jnp.max(scores, axis=1, keepdims=True), own)
    expo = jnp.exp(scores - top)
    own_expo = jnp.exp(own - top)
    total = jnp.sum(expo, axis=1, keepdims=True) + own_expo
    weights = (expo / total).astype(BF16)
    own_weight = (own_expo / total).astype(BF16).astype(F32)

    copies[5].wait()
    parts = []
    for p in range(seqs // 2):
        v_pair = jnp.concatenate([vbuf[2 * p], vbuf[2 * p + 1]], axis=1)
        both = dot(weights[16 * p:16 * p + 16], v_pair)
        parts.append(both[:8, :128])
        parts.append(both[8:, 128:])
    out = jnp.concatenate(parts, axis=0) + own_weight * value_rows
    out = jnp.where(half == kv_half, out, 0.0)
    out_turned = pltpu.roll(out, HEAD_DIM, 1)
    outs = []
    for b in range(HEADS // 2):
        piece = jnp.where(head // 2 == b, jnp.where(head % 2 == kv_half, out, out_turned), 0.0)
        outs.append(lax.dot_general(spread, piece.astype(BF16), TN, preferred_element_type=F32))
    attended = jnp.concatenate(outs, axis=1).astype(BF16)
    copies[6].wait()
    mixed = (x + dot(attended, wo[...])).astype(BF16)
    mixed_ref[...] = mixed
    y = mixed.astype(F32)
    scale = lax.rsqrt(jnp.mean(y * y, axis=1, keepdims=True) + EPS)
    routed_in = (y * scale * egain_ref[...]).astype(BF16)
    branch = jax.nn.sigmoid(jnp.sum(routed_in.astype(F32) * bgate_ref[...], axis=1, keepdims=True))
    branch_ref[...] = jnp.broadcast_to(branch, branch_ref.shape)
    fill_outgoing(routed_in, ids_ref, eweights_ref, place_ref, outgoing_ref)


def mixer(tokens, attn_norm_gain, w_query, w_key, w_value, w_forget, forget_bias, w_attn_out,
          cache_keys, cache_values, cache_logcum, cache_lengths, expert_norm_gain, branch_gate,
          expert_ids, expert_weights, devices):
    seqs, width = tokens.shape
    length = cache_keys.shape[1]
    return pl.pallas_call(
        mixer_body,
        out_shape=(
            jax.ShapeDtypeStruct((seqs, width), BF16),
            jax.ShapeDtypeStruct((seqs, 128), F32),
            jax.ShapeDtypeStruct((devices * CAP, seqs), F32),
            jax.ShapeDtypeStruct((devices, CAP, 2 * width + width // CAP), BF16),
        ),
        in_specs=[VMEM, VMEM, ANY, ANY, ANY, VMEM, VMEM, ANY, ANY, ANY, ANY, VMEM, VMEM, VMEM, VMEM, VMEM],
        out_specs=(VMEM, VMEM, VMEM, VMEM),
        scratch_shapes=[
            pltpu.VMEM(w_query.shape, BF16),
            pltpu.VMEM(w_key.shape, BF16),
            pltpu.VMEM(w_value.shape, BF16),
            pltpu.VMEM(w_attn_out.shape, BF16),
            pltpu.VMEM(cache_keys.shape, BF16),
            pltpu.VMEM(cache_values.shape, BF16),
            pltpu.VMEM(cache_logcum.shape, F32),
            pltpu.SemaphoreType.DMA((7,)),
        ],
        compiler_params=pltpu.CompilerParams(vmem_limit_bytes=40 * 1024 * 1024),
        name="mixer",
    )(tokens, attn_norm_gain.reshape(1, width), w_query, w_key, w_value, w_forget.T,
      forget_bias.reshape(1, HEADS), w_attn_out, cache_keys, cache_values, cache_logcum,
      cache_lengths.reshape(1, seqs), expert_norm_gain.reshape(1, width),
      branch_gate.reshape(1, width), expert_ids.T, expert_weights.T)


def pair(a):
    return a.reshape(a.shape[0] // CAP, CAP, a.shape[1])


def worker_body(
    device_ref, arrived_ref, gate_hbm, up_hbm, down_hbm,
    p0, p1, p2, p3, p4, p5, p6, p7, gain_ref,
    answer_ref, wg, wu, wd, sems,
):
    devices, cap, packed = arrived_ref.shape
    rows = devices * cap
    width = wd.shape[1]
    half = width // CAP
    copies = [
        pltpu.make_async_copy(gate_hbm.at[0], wg, sems.at[0]),
        pltpu.make_async_copy(up_hbm.at[0], wu, sems.at[1]),
        pltpu.make_async_copy(down_hbm.at[0], wd, sems.at[2]),
    ]
    for copy in copies:
        copy.start()
    pieces = (p0, p1, p2, p3, p4, p5, p6, p7)
    units = pieces[0].shape[0] // 3
    me = device_ref[0]
    gains = []
    lane = lax.broadcasted_iota(jnp.int32, (1, 128), 1)
    per_row = 128 // units
    for block in range(PARTS // per_row):
        vec = jnp.zeros((1, 128), F32)
        for q in range(per_row):
            p = block * per_row + q
            owner = lax.rem(me + (PARTS // CORES - p // CORES) * PLANE, devices)
            if p % CORES:
                owner = owner + 1 - 2 * lax.rem(me, CORES)
            line = gain_ref[pl.ds(owner // per_row, 1), :]
            shift = lax.rem(q - lax.rem(owner, per_row) + per_row, per_row) * units
            vec = jnp.where(lane // units == q, pltpu.roll(line, shift, 1), vec)
        gains.append(vec)
    gain = jnp.concatenate(gains, axis=1)
    dg = jnp.concatenate([r[:units] for r in pieces], axis=0)
    du = jnp.concatenate([r[units:2 * units] for r in pieces], axis=0)
    dd = jnp.concatenate([r[2 * units:] for r in pieces], axis=0)

    def nt(a, b):
        return lax.dot_general(a, b, NT, preferred_element_type=F32)

    def hidden_of(gate, up):
        kept = (jax.nn.silu(gate) * up).astype(BF16).astype(F32)
        square = jnp.sum(kept * kept, axis=1, keepdims=True)
        return (kept * gain).astype(BF16), square

    first = arrived_ref[:, :, width:2 * width].reshape(rows, width)
    extra = arrived_ref[:, :, 2 * width:].reshape(rows, half)
    hid, square = hidden_of(nt(first, dg), nt(first, du))
    answer_ref[:, :, width:2 * width] = pair(dot(hid, dd).astype(BF16))
    even = lax.broadcasted_iota(jnp.int32, (rows, PARTS * units), 0) % CAP == 0

    def joined(weight):
        both = jnp.where(even, nt(extra, weight[:, :half]), nt(extra, weight[:, half:]))
        return both + pltpu.roll(both, rows - 1, 0)

    hid3, square3 = hidden_of(joined(dg), joined(du))
    low = dot(hid3, dd[:, :half])
    high = pltpu.roll(dot(hid3, dd[:, half:]), 1, 0)
    even = lax.broadcasted_iota(jnp.int32, (rows, half), 0) % CAP == 0
    answer_ref[:, :, 2 * width:2 * width + half] = pair(jnp.where(even, low, high).astype(BF16))
    lane = lax.broadcasted_iota(jnp.int32, (rows, 128), 1)
    head = jnp.where(lane < 2, square, square3)
    top = head.astype(BF16).astype(F32)
    tail = jnp.where(lane % 2 == 0, top, head - top)
    answer_ref[:, :, 2 * width + half:] = pair(jnp.where(lane < 4, tail, 0.0).astype(BF16))

    x = arrived_ref[:, :, :width].reshape(rows, width)
    copies[0].wait()
    gate = jnp.minimum(dot(x, wg[...]), LIMIT)
    copies[1].wait()
    up = jnp.clip(dot(x, wu[...]), -LIMIT, LIMIT)
    act = ((up + 1.0) * gate * jax.nn.sigmoid(gate * ALPHA)).astype(BF16)
    copies[2].wait()
    answer_ref[:, :, :width] = pair(dot(act, wd[...]).astype(BF16))


def worker(device, arrived, gate_w, up_w, down_w, pieces, gain):
    devices, cap, packed = arrived.shape
    return pl.pallas_call(
        worker_body,
        out_shape=jax.ShapeDtypeStruct((devices, cap, packed + 128), BF16),
        in_specs=[pl.BlockSpec(memory_space=pltpu.SMEM), VMEM, ANY, ANY, ANY] + [VMEM] * 9,
        out_specs=VMEM,
        scratch_shapes=[
            pltpu.VMEM(gate_w.shape[1:], BF16),
            pltpu.VMEM(up_w.shape[1:], BF16),
            pltpu.VMEM(down_w.shape[1:], BF16),
            pltpu.SemaphoreType.DMA((3,)),
        ],
        compiler_params=pltpu.CompilerParams(vmem_limit_bytes=48 * 1024 * 1024),
        name="worker",
    )(device, arrived, gate_w, up_w, down_w, *pieces, gain.reshape(-1, 128))


def merger_body(returned_ref, place_ref, mixed_ref, branch_ref, result_ref):
    devices, cap, packed = returned_ref.shape
    seqs, width = mixed_ref.shape
    rows = devices * cap
    half = width // CAP

    def tn(a, b):
        return lax.dot_general(a, b, TN, preferred_element_type=F32)

    slot, device, dense, extra = slot_masks(rows, seqs)
    share = place_ref[...]
    s1 = share.astype(BF16)
    rest = share - s1.astype(F32)
    s2 = rest.astype(BF16)
    s3 = (rest - s2.astype(F32)).astype(BF16)
    answers = returned_ref[:, :, :width].reshape(rows, width)
    routed = tn(s1, answers) + tn(s2, answers) + tn(s3, answers)
    dense = jnp.where(dense, 1.0, 0.0).astype(BF16)
    low = jnp.where(extra & (slot % CAP == 0), 1.0, 0.0).astype(BF16)
    high = jnp.where(extra & (slot % CAP == 1), 1.0, 0.0).astype(BF16)
    total = tn(dense, returned_ref[:, :, width:2 * width].reshape(rows, width))
    third = returned_ref[:, :, 2 * width:2 * width + half].reshape(rows, half)
    total = total + jnp.concatenate([tn(low, third), tn(high, third)], axis=1)
    sums = returned_ref[:, :, 2 * width + half:].reshape(rows, 128)
    lane = lax.broadcasted_iota(jnp.int32, (seqs, 128), 1)
    square = jnp.where(lane < 2, tn(dense, sums), 0.0)
    square = square + jnp.where((lane >= 2) & (lane < 4), tn(low, sums), 0.0)
    square = jnp.sum(square, axis=1, keepdims=True)
    unit_scale = lax.rsqrt(square / DENSE_FF + EPS)
    out = mixed_ref[...].astype(F32) + routed + branch_ref[:, :1] * (total * unit_scale)
    result_ref[...] = out.astype(BF16)


def merger(returned, place, mixed, branch):
    return pl.pallas_call(
        merger_body,
        out_shape=jax.ShapeDtypeStruct(mixed.shape, BF16),
        in_specs=[VMEM] * 4,
        out_specs=VMEM,
        compiler_params=pltpu.CompilerParams(vmem_limit_bytes=32 * 1024 * 1024),
        name="merger",
    )(returned, place, mixed, branch)


def gather_pieces(own, devices):
    def moved(array, target):
        return lax.ppermute(array, "ep", [(d, target(d)) for d in range(devices)])

    pieces = []
    for hop in range(PARTS // CORES):
        mine = own if hop == 0 else moved(own, lambda d: (d + hop * PLANE) % devices)
        pieces.append(mine)
        pieces.append(moved(mine, lambda d: d ^ 1))
    return pieces


def shards(
    tokens, attn_norm_gain, w_query, w_key, w_value, w_forget, forget_bias, w_attn_out,
    cache_keys, cache_values, cache_logcum, cache_lengths, expert_norm_gain, expert_ids,
    expert_weights, w_expert_gate, w_expert_up, w_expert_down, w_dense_gate, w_dense_up,
    w_dense_down, dense_norm_gain, branch_gate,
):
    devices = lax.axis_size("ep")
    own = jnp.concatenate([w_dense_gate.T, w_dense_up.T, w_dense_down], axis=0)
    pieces = gather_pieces(own, devices)
    mixed, branch, place, outgoing = mixer(
        tokens, attn_norm_gain, w_query, w_key, w_value, w_forget, forget_bias, w_attn_out,
        cache_keys, cache_values, cache_logcum, cache_lengths, expert_norm_gain, branch_gate,
        expert_ids, expert_weights, devices)
    arrived = lax.all_to_all(outgoing, "ep", split_axis=0, concat_axis=0, tiled=True)
    me = lax.axis_index("ep").astype(jnp.int32).reshape(1)
    answer = worker(me, arrived, w_expert_gate, w_expert_up, w_expert_down, pieces, dense_norm_gain)
    returned = lax.all_to_all(answer, "ep", split_axis=0, concat_axis=0, tiled=True)
    return merger(returned, place, mixed, branch)


def solution(mesh):
    in_specs = (
        P("ep", None),
        P(),
        P(),
        P(),
        P(),
        P(),
        P(),
        P(),
        P("ep", None, None),
        P("ep", None, None),
        P("ep", None, None),
        P("ep"),
        P(),
        P("ep", None),
        P("ep", None),
        P("ep", None, None),
        P("ep", None, None),
        P("ep", None, None),
        P(None, "ep"),
        P(None, "ep"),
        P("ep", None),
        P(),
        P(),
    )
    out_specs = P("ep", None)
    return jax.shard_map(shards, mesh=mesh, in_specs=in_specs, out_specs=out_specs, check_vma=False)
```

```python
import jax
import jax.numpy as jnp
from jax import lax
from jax.experimental import pallas as pl
from jax.experimental.pallas import tpu as pltpu
from jax.sharding import PartitionSpec as P


HEADS = 8
KV_HEADS = 2
HEAD_DIM = 64
TOPK = 6
EPS = 1e-06
LIMIT = 7.0
ALPHA = 1.702
CAP = 2
PLANE = 32
CORES = 2
PARTS = 8
DENSE_FF = 4096
F32 = jnp.float32
BF16 = jnp.bfloat16
VMEM = pl.BlockSpec(memory_space=pltpu.VMEM)
HBM = pl.BlockSpec(memory_space=pltpu.HBM)
NT = (((1,), (1,)), ((), ()))
TN = (((0,), (0,)), ((), ()))


def dot(a, b):
    return jnp.dot(a, b, preferred_element_type=F32)


def slot_masks(slots, seqs):
    slot = lax.broadcasted_iota(jnp.int32, (slots, seqs), 0)
    token = lax.broadcasted_iota(jnp.int32, (slots, seqs), 1)
    device = slot // CAP
    part = (device // PLANE) * CORES + device % CORES
    dense = token == part + PARTS * (slot % CAP)
    extra = token == part + PARTS * CAP
    return slot, device, dense, extra


def fill_outgoing(
    routed_in, ids_ref, eweights_ref, place_ref, outgoing_ref, outgoing_hbm, out_sems
):
    seqs, width = routed_in.shape
    half = width // CAP
    slots = outgoing_ref.shape[0] * CAP
    slot, device, dense, extra = slot_masks(slots, seqs)
    member = jnp.zeros((slots, seqs), F32)
    share = jnp.zeros((slots, seqs), F32)
    for k in range(TOPK):
        hit = ids_ref[k:k + 1, :] == device
        member = member + jnp.where(hit, 1.0, 0.0)
        share = share + jnp.where(hit, eweights_ref[k:k + 1, :], 0.0)
    earlier = lax.broadcasted_iota(jnp.int32, (seqs, seqs), 0)
    later = lax.broadcasted_iota(jnp.int32, (seqs, seqs), 1)
    before = jnp.where(earlier < later, 1.0, 0.0).astype(BF16)
    prior = dot(member.astype(BF16), before)
    here = prior == (slot % CAP).astype(F32)
    place_ref[...] = jnp.where(here, share, 0.0)
    routes = jnp.where(here, member, 0.0).astype(BF16)
    extra = jnp.where(extra, 1.0, 0.0).astype(BF16)
    even = lax.broadcasted_iota(jnp.int32, (slots, half), 0) % CAP == 0
    third = jnp.where(even, dot(extra, routed_in[:, :half]), dot(extra, routed_in[:, half:]))
    devices = slots // CAP
    copies = []

    def send(start, stop, value):
        window = (slice(None), slice(None), pl.ds(start, stop - start))
        outgoing_ref[window] = value.astype(BF16).reshape(devices, CAP, stop - start)
        copies.append(pltpu.make_async_copy(
            outgoing_ref.at[window], outgoing_hbm.at[window], out_sems.at[len(copies)]))
        copies[-1].start()

    send(2 * width, 2 * width + half, third)
    send(width, 2 * width, dot(jnp.where(dense, 1.0, 0.0).astype(BF16), routed_in))
    send(0, width, dot(routes, routed_in))
    for copy in copies:
        copy.wait()


def mixer_body(
    tokens_hbm, again_hbm, wq_hbm, wk_hbm, wv_hbm, wf_hbm, fbias_hbm, wo_hbm,
    keys_hbm, values_hbm, logcum_hbm, lengths_hbm, egain_hbm, bgate_hbm, ids_hbm, eweights_hbm,
    mixed_ref, branch_ref, place_ref, outgoing_hbm,
    tokens_ref, again_ref, wq, wk, wv, wf_ref, fbias_ref, wo,
    kbuf, vbuf, cbuf, lengths_ref, egain_ref, bgate_ref, ids_ref, eweights_ref, sems,
    outgoing_ref, out_sems,
):
    sources = dict(
        tokens=(tokens_hbm, tokens_ref), again=(again_hbm, again_ref), wf=(wf_hbm, wf_ref),
        fbias=(fbias_hbm, fbias_ref), lengths=(lengths_hbm, lengths_ref), wq=(wq_hbm, wq),
        wk=(wk_hbm, wk), wv=(wv_hbm, wv), keys=(keys_hbm, kbuf), logcum=(logcum_hbm, cbuf),
        values=(values_hbm, vbuf), wo=(wo_hbm, wo), egain=(egain_hbm, egain_ref),
        bgate=(bgate_hbm, bgate_ref), ids=(ids_hbm, ids_ref), eweights=(eweights_hbm, eweights_ref))
    copies = {}
    for i, (name, (source, target)) in enumerate(sources.items()):
        copies[name] = pltpu.make_async_copy(source, target, sems.at[i])
        copies[name].start()

    def ready(*names):
        for name in names:
            copies[name].wait()

    seqs, _ = tokens_ref.shape
    length = kbuf.shape[1]
    rows = seqs * HEADS
    ready("tokens", "again", "wf", "fbias", "lengths")
    x = tokens_ref[...].astype(F32)
    scale = lax.rsqrt(jnp.mean(x * x, axis=1, keepdims=True) + EPS)
    normed = (x * scale * again_ref[...]).astype(BF16)
    forget = lax.dot_general(normed, wf_ref[...], NT, preferred_element_type=F32) + fbias_ref[...]
    log_forget = jax.nn.log_sigmoid(forget)
    row = lax.broadcasted_iota(jnp.int32, (rows, seqs), 0)
    col = lax.broadcasted_iota(jnp.int32, (rows, seqs), 1)
    spread_mask = (row // HEADS) == col
    spread = jnp.where(spread_mask, 1.0, 0.0).astype(BF16)
    live_len = jnp.sum(jnp.where(spread_mask, lengths_ref[...], 0), axis=1, keepdims=True)
    head8 = lax.broadcasted_iota(jnp.int32, (rows, HEADS), 0) % HEADS
    lane8 = lax.broadcasted_iota(jnp.int32, (rows, HEADS), 1)
    lf_rows = lax.dot_general(
        jnp.where(spread_mask, 1.0, 0.0), log_forget, (((1,), (0,)), ((), ())),
        precision=lax.Precision.HIGHEST, preferred_element_type=F32)
    lf_rows = jnp.sum(jnp.where(head8 == lane8, lf_rows, 0.0), axis=1, keepdims=True)

    ready("wq", "wk", "wv")
    query = dot(normed, wq[...]).astype(BF16)
    key_new = dot(normed, wk[...]).astype(BF16)
    value_new = dot(normed, wv[...]).astype(BF16)
    q_rows = dot(spread, query)
    key_rows = dot(spread, key_new)
    value_rows = dot(spread, value_new)
    head = lax.broadcasted_iota(jnp.int32, (rows, 128), 0) % HEADS
    lane = lax.broadcasted_iota(jnp.int32, (rows, 128), 1)
    half = lane // HEAD_DIM
    kv_half = head // (HEADS // KV_HEADS)
    q_sel = jnp.zeros((rows, 128), F32)
    for b in range(HEADS // 2):
        block = q_rows[:, 128 * b:128 * b + 128]
        turned = pltpu.roll(block, HEAD_DIM, 1)
        q_sel = jnp.where(head // 2 == b, jnp.where(head % 2 == kv_half, block, turned), q_sel)
    q_sel = jnp.where(half == kv_half, q_sel, 0.0)
    own = jnp.sum(q_sel * key_rows, axis=1, keepdims=True) * (HEAD_DIM ** -0.5)
    q_bf = q_sel.astype(BF16)
    seq_row = lax.broadcasted_iota(jnp.int32, (rows, 128), 0) // HEADS
    blocks = [jnp.where(seq_row == s, q_sel, 0.0).astype(BF16) for s in range(seqs)]
    q_block = jnp.concatenate(blocks, axis=1)

    ready("keys")
    k_all = jnp.concatenate([kbuf[s] for s in range(seqs)], axis=1)
    scores_t = lax.dot_general(k_all, q_block, NT, preferred_element_type=F32)
    scores = jnp.transpose(scores_t)
    ready("logcum")
    logcum = cbuf[...].reshape(rows, length)
    place = lax.broadcasted_iota(jnp.int32, (rows, length), 1)
    last = jnp.sum(jnp.where(place == live_len - 1, logcum, 0.0), axis=1, keepdims=True)
    carried = last + lf_rows
    scores = scores * (HEAD_DIM ** -0.5) + (carried - logcum)
    scores = jnp.where(place < live_len, scores, -jnp.inf)
    top = jnp.maximum(jnp.max(scores, axis=1, keepdims=True), own)
    expo = jnp.exp(scores - top)
    own_expo = jnp.exp(own - top)
    total = jnp.sum(expo, axis=1, keepdims=True) + own_expo
    weights = (expo / total).astype(BF16)
    own_weight = (own_expo / total).astype(BF16).astype(F32)

    ready("values")
    parts = []
    for p in range(seqs // 2):
        v_pair = jnp.concatenate([vbuf[2 * p], vbuf[2 * p + 1]], axis=1)
        both = dot(weights[16 * p:16 * p + 16], v_pair)
        parts.append(both[:8, :128])
        parts.append(both[8:, 128:])
    out = jnp.concatenate(parts, axis=0) + own_weight * value_rows
    out = jnp.where(half == kv_half, out, 0.0)
    out_turned = pltpu.roll(out, HEAD_DIM, 1)
    outs = []
    for b in range(HEADS // 2):
        piece = jnp.where(head // 2 == b, jnp.where(head % 2 == kv_half, out, out_turned), 0.0)
        outs.append(lax.dot_general(spread, piece.astype(BF16), TN, preferred_element_type=F32))
    attended = jnp.concatenate(outs, axis=1).astype(BF16)
    ready("wo", "egain", "bgate", "ids", "eweights")
    mixed = (x + dot(attended, wo[...])).astype(BF16)
    mixed_ref[...] = mixed
    y = mixed.astype(F32)
    scale = lax.rsqrt(jnp.mean(y * y, axis=1, keepdims=True) + EPS)
    routed_in = (y * scale * egain_ref[...]).astype(BF16)
    branch = jax.nn.sigmoid(jnp.sum(routed_in.astype(F32) * bgate_ref[...], axis=1, keepdims=True))
    branch_ref[...] = jnp.broadcast_to(branch, branch_ref.shape)
    fill_outgoing(
        routed_in, ids_ref, eweights_ref, place_ref, outgoing_ref, outgoing_hbm, out_sems)


def mixer(tokens, attn_norm_gain, w_query, w_key, w_value, w_forget, forget_bias, w_attn_out,
          cache_keys, cache_values, cache_logcum, cache_lengths, expert_norm_gain, branch_gate,
          expert_ids, expert_weights, devices):
    seqs, width = tokens.shape
    operands = (
        tokens, attn_norm_gain.reshape(1, width), w_query, w_key, w_value, w_forget.T,
        forget_bias.reshape(1, HEADS), w_attn_out, cache_keys, cache_values, cache_logcum,
        cache_lengths.reshape(1, seqs), expert_norm_gain.reshape(1, width),
        branch_gate.reshape(1, width), expert_ids.T, expert_weights.T)
    operands = tuple(pltpu.with_memory_space_constraint(a, pltpu.HBM) for a in operands)
    return pl.pallas_call(
        mixer_body,
        out_shape=(
            jax.ShapeDtypeStruct((seqs, width), BF16),
            jax.ShapeDtypeStruct((seqs, 128), F32),
            jax.ShapeDtypeStruct((devices * CAP, seqs), F32),
            pltpu.HBM((devices, CAP, 2 * width + width // CAP), BF16),
        ),
        in_specs=[HBM] * len(operands),
        out_specs=(VMEM, VMEM, VMEM, HBM),
        scratch_shapes=[pltpu.VMEM(a.shape, a.dtype) for a in operands]
        + [
            pltpu.SemaphoreType.DMA((len(operands),)),
            pltpu.VMEM((devices, CAP, 2 * width + width // CAP), BF16),
            pltpu.SemaphoreType.DMA((3,)),
        ],
        compiler_params=pltpu.CompilerParams(vmem_limit_bytes=28 * 1024 * 1024),
        cost_estimate=pl.CostEstimate(flops=10**10, bytes_accessed=15 * 2**20, transcendentals=0),
        name="mixer",
    )(*operands)


def pair(a):
    return a.reshape(a.shape[0] // CAP, CAP, a.shape[1])


def worker_body(
    device_ref, arrived_ref, gate_hbm, up_hbm, down_hbm,
    h0, h1, h2, h3, h4, h5, h6, h7, gain_ref,
    answer_ref, wg, wu, wd, held, sems,
):
    devices, cap, _ = arrived_ref.shape
    rows = devices * cap
    width = wd.shape[1]
    half = width // CAP
    weight_copies = [
        pltpu.make_async_copy(source.at[0], target, sems.at[i])
        for i, (source, target) in enumerate(((gate_hbm, wg), (up_hbm, wu), (down_hbm, wd)))]
    piece_copies = [
        pltpu.make_async_copy(source, held.at[i], sems.at[3 + i])
        for i, source in enumerate((h0, h1, h2, h3, h4, h5, h6, h7))]
    for copy in weight_copies + piece_copies:
        copy.start()
    x = arrived_ref[:, :, :width].reshape(rows, width)
    weight_copies[0].wait()
    gate = jnp.minimum(dot(x, wg[...]), LIMIT)
    weight_copies[1].wait()
    up = jnp.clip(dot(x, wu[...]), -LIMIT, LIMIT)
    act = ((up + 1.0) * gate * jax.nn.sigmoid(gate * ALPHA)).astype(BF16)
    weight_copies[2].wait()
    answer_ref[:, :, :width] = pair(dot(act, wd[...]).astype(BF16))

    units = held.shape[1] // 3
    me = device_ref[0]
    gains = []
    lane = lax.broadcasted_iota(jnp.int32, (1, 128), 1)
    per_row = 128 // units
    for block in range(PARTS // per_row):
        vec = jnp.zeros((1, 128), F32)
        for q in range(per_row):
            p = block * per_row + q
            owner = lax.rem(me + (PARTS // CORES - p // CORES) * PLANE, devices)
            if p % CORES:
                owner = owner + 1 - 2 * lax.rem(me, CORES)
            line = gain_ref[pl.ds(owner // per_row, 1), :]
            shift = lax.rem(q - lax.rem(owner, per_row) + per_row, per_row) * units
            vec = jnp.where(lane // units == q, pltpu.roll(line, shift, 1), vec)
        gains.append(vec)
    gain = jnp.concatenate(gains, axis=1)
    for copy in piece_copies:
        copy.wait()
    dg = jnp.concatenate([held[p, :units] for p in range(PARTS)], axis=0)
    du = jnp.concatenate([held[p, units:2 * units] for p in range(PARTS)], axis=0)
    dd = jnp.concatenate([held[p, 2 * units:] for p in range(PARTS)], axis=0)

    def nt(a, b):
        return lax.dot_general(a, b, NT, preferred_element_type=F32)

    def hidden_of(gate, up):
        kept = (jax.nn.silu(gate) * up).astype(BF16).astype(F32)
        square = jnp.sum(kept * kept, axis=1, keepdims=True)
        return (kept * gain).astype(BF16), square

    first = arrived_ref[:, :, width:2 * width].reshape(rows, width)
    extra = arrived_ref[:, :, 2 * width:].reshape(rows, half)
    hid, square = hidden_of(nt(first, dg), nt(first, du))
    answer_ref[:, :, width:2 * width] = pair(dot(hid, dd).astype(BF16))
    even = lax.broadcasted_iota(jnp.int32, (rows, PARTS * units), 0) % CAP == 0

    def joined(weight):
        both = jnp.where(even, nt(extra, weight[:, :half]), nt(extra, weight[:, half:]))
        return both + pltpu.roll(both, rows - 1, 0)

    hid3, square3 = hidden_of(joined(dg), joined(du))
    low = dot(hid3, dd[:, :half])
    high = pltpu.roll(dot(hid3, dd[:, half:]), 1, 0)
    even = lax.broadcasted_iota(jnp.int32, (rows, half), 0) % CAP == 0
    answer_ref[:, :, 2 * width:2 * width + half] = pair(jnp.where(even, low, high).astype(BF16))
    lane = lax.broadcasted_iota(jnp.int32, (rows, 128), 1)
    head = jnp.where(lane < 2, square, square3)
    top = head.astype(BF16).astype(F32)
    tail = jnp.where(lane % 2 == 0, top, head - top)
    answer_ref[:, :, 2 * width + half:] = pair(jnp.where(lane < 4, tail, 0.0).astype(BF16))


def worker(device, arrived, gate_w, up_w, down_w, pieces, gain):
    devices, cap, packed = arrived.shape
    stored = tuple(
        pltpu.with_memory_space_constraint(a, pltpu.HBM) for a in (gate_w, up_w, down_w))
    pieces = tuple(pltpu.with_memory_space_constraint(a, pltpu.HBM) for a in pieces)
    return pl.pallas_call(
        worker_body,
        out_shape=jax.ShapeDtypeStruct((devices, cap, packed + 128), BF16),
        in_specs=[pl.BlockSpec(memory_space=pltpu.SMEM), VMEM] + [HBM] * 11 + [VMEM],
        out_specs=VMEM,
        scratch_shapes=[pltpu.VMEM(a.shape[1:], BF16) for a in stored]
        + [
            pltpu.VMEM((len(pieces),) + pieces[0].shape, BF16),
            pltpu.SemaphoreType.DMA((3 + len(pieces),)),
        ],
        compiler_params=pltpu.CompilerParams(vmem_limit_bytes=28 * 1024 * 1024),
        cost_estimate=pl.CostEstimate(flops=5 * 10**9, bytes_accessed=15 * 2**20, transcendentals=0),
        name="worker",
    )(device, arrived, *stored, *pieces, gain.reshape(-1, 128))


def merger_body(returned_ref, place_ref, mixed_ref, branch_ref, result_ref):
    devices, cap, _ = returned_ref.shape
    seqs, width = mixed_ref.shape
    rows = devices * cap
    half = width // CAP

    def tn(a, b):
        return lax.dot_general(a, b, TN, preferred_element_type=F32)

    slot, _, dense, extra = slot_masks(rows, seqs)
    share = place_ref[...]
    s1 = share.astype(BF16)
    rest = share - s1.astype(F32)
    s2 = rest.astype(BF16)
    s3 = (rest - s2.astype(F32)).astype(BF16)
    answers = returned_ref[:, :, :width].reshape(rows, width)
    routed = tn(s1, answers) + tn(s2, answers) + tn(s3, answers)
    dense = jnp.where(dense, 1.0, 0.0).astype(BF16)
    low = jnp.where(extra & (slot % CAP == 0), 1.0, 0.0).astype(BF16)
    high = jnp.where(extra & (slot % CAP == 1), 1.0, 0.0).astype(BF16)
    total = tn(dense, returned_ref[:, :, width:2 * width].reshape(rows, width))
    third = returned_ref[:, :, 2 * width:2 * width + half].reshape(rows, half)
    total = total + jnp.concatenate([tn(low, third), tn(high, third)], axis=1)
    sums = returned_ref[:, :, 2 * width + half:].reshape(rows, 128)
    lane = lax.broadcasted_iota(jnp.int32, (seqs, 128), 1)
    square = jnp.where(lane < 2, tn(dense, sums), 0.0)
    square = square + jnp.where((lane >= 2) & (lane < 4), tn(low, sums), 0.0)
    square = jnp.sum(square, axis=1, keepdims=True)
    unit_scale = lax.rsqrt(square / DENSE_FF + EPS)
    out = mixed_ref[...].astype(F32) + routed + branch_ref[:, :1] * (total * unit_scale)
    result_ref[...] = out.astype(BF16)


def merger(returned, place, mixed, branch):
    return pl.pallas_call(
        merger_body,
        out_shape=jax.ShapeDtypeStruct(mixed.shape, BF16),
        in_specs=[VMEM] * 4,
        out_specs=VMEM,
        compiler_params=pltpu.CompilerParams(vmem_limit_bytes=16 * 1024 * 1024),
        name="merger",
    )(returned, place, mixed, branch)


def gather_pieces(own, devices):
    def moved(array, target):
        return lax.ppermute(array, "ep", [(d, target(d)) for d in range(devices)])

    pieces = []
    for hop in range(PARTS // CORES):
        mine = own
        if hop:
            mine = moved(own, lambda d: (d + hop * PLANE) % devices)
        pieces.append(mine)
        pieces.append(moved(mine, lambda d: d ^ 1))
    return pieces


def layer(
    tokens, attn_norm_gain, w_query, w_key, w_value, w_forget, forget_bias, w_attn_out,
    cache_keys, cache_values, cache_logcum, cache_lengths, expert_norm_gain, expert_ids,
    expert_weights, w_expert_gate, w_expert_up, w_expert_down, w_dense_gate, w_dense_up,
    w_dense_down, dense_norm_gain, branch_gate,
):
    devices = lax.axis_size("ep")
    own = jnp.concatenate([w_dense_gate.T, w_dense_up.T, w_dense_down], axis=0)
    pieces = gather_pieces(own, devices)
    mixed, branch, place, outgoing = mixer(
        tokens, attn_norm_gain, w_query, w_key, w_value, w_forget, forget_bias, w_attn_out,
        cache_keys, cache_values, cache_logcum, cache_lengths, expert_norm_gain, branch_gate,
        expert_ids, expert_weights, devices)
    arrived = lax.all_to_all(outgoing, "ep", split_axis=0, concat_axis=0, tiled=True)
    me = lax.axis_index("ep").astype(jnp.int32).reshape(1)
    answer = worker(me, arrived, w_expert_gate, w_expert_up, w_expert_down, pieces, dense_norm_gain)
    returned = lax.all_to_all(answer, "ep", split_axis=0, concat_axis=0, tiled=True)
    return merger(returned, place, mixed, branch)


def solution(mesh):
    in_specs = (
        P("ep", None),
        P(),
        P(),
        P(),
        P(),
        P(),
        P(),
        P(),
        P("ep", None, None),
        P("ep", None, None),
        P("ep", None, None),
        P("ep"),
        P(),
        P("ep", None),
        P("ep", None),
        P("ep", None, None),
        P("ep", None, None),
        P("ep", None, None),
        P(None, "ep"),
        P(None, "ep"),
        P("ep", None),
        P(),
        P(),
    )
    out_specs = P("ep", None)
    return jax.shard_map(
        layer, mesh=mesh, in_specs=in_specs, out_specs=out_specs, check_vma=False)
```

```python
import jax
import jax.numpy as jnp
from jax import lax
from jax.experimental import pallas as pl
from jax.experimental.pallas import tpu as pltpu
from jax.sharding import PartitionSpec as P


HEADS = 8
KV_HEADS = 2
HEAD_DIM = 64
TOPK = 6
EPS = 1e-06
LIMIT = 7.0
ALPHA = 1.702
CAP = 2
PLANE = 32
CORES = 2
PARTS = 8
SIDE = 4
DENSE_FF = 4096
F32 = jnp.float32
BF16 = jnp.bfloat16
VMEM = pl.BlockSpec(memory_space=pltpu.VMEM)
HBM = pl.BlockSpec(memory_space=pltpu.HBM)
NT = (((1,), (1,)), ((), ()))
TN = (((0,), (0,)), ((), ()))


def dot(a, b):
    return jnp.dot(a, b, preferred_element_type=F32)


def fill_outgoing(routed_in, ids_ref, eweights_ref, place_ref, outgoing_ref):
    seqs, width = routed_in.shape
    devices = outgoing_ref.shape[0]
    slots = devices * CAP
    slot = lax.broadcasted_iota(jnp.int32, (slots, seqs), 0)
    member = jnp.zeros((slots, seqs), F32)
    share = jnp.zeros((slots, seqs), F32)
    for k in range(TOPK):
        hit = ids_ref[k:k + 1, :] == slot // CAP
        member = member + jnp.where(hit, 1.0, 0.0)
        share = share + jnp.where(hit, eweights_ref[k:k + 1, :], 0.0)
    earlier = lax.broadcasted_iota(jnp.int32, (seqs, seqs), 0)
    later = lax.broadcasted_iota(jnp.int32, (seqs, seqs), 1)
    before = jnp.where(earlier < later, 1.0, 0.0).astype(BF16)
    prior = dot(member.astype(BF16), before)
    here = prior == (slot % CAP).astype(F32)
    place_ref[...] = jnp.where(here, share, 0.0)
    routes = jnp.where(here, member, 0.0).astype(BF16)
    outgoing_ref[...] = dot(routes, routed_in).astype(BF16).reshape(devices, CAP, width)


def mixer_body(
    tokens_hbm, again_hbm, wq_hbm, wk_hbm, wv_hbm, wf_hbm, fbias_hbm, wo_hbm,
    keys_hbm, values_hbm, logcum_hbm, lengths_hbm, egain_hbm, bgate_hbm, ids_hbm, eweights_hbm,
    mixed_ref, routed_ref, branch_ref, place_ref, outgoing_ref,
    tokens_ref, again_ref, wq, wk, wv, wf_ref, fbias_ref, wo,
    kbuf, vbuf, cbuf, lengths_ref, egain_ref, bgate_ref, ids_ref, eweights_ref, sems,
):
    sources = dict(
        tokens=(tokens_hbm, tokens_ref), again=(again_hbm, again_ref), wf=(wf_hbm, wf_ref),
        fbias=(fbias_hbm, fbias_ref), lengths=(lengths_hbm, lengths_ref), wq=(wq_hbm, wq),
        wk=(wk_hbm, wk), wv=(wv_hbm, wv), keys=(keys_hbm, kbuf), logcum=(logcum_hbm, cbuf),
        values=(values_hbm, vbuf), wo=(wo_hbm, wo), egain=(egain_hbm, egain_ref),
        bgate=(bgate_hbm, bgate_ref), ids=(ids_hbm, ids_ref), eweights=(eweights_hbm, eweights_ref))
    copies = {}
    for i, (name, (source, target)) in enumerate(sources.items()):
        copies[name] = pltpu.make_async_copy(source, target, sems.at[i])
        copies[name].start()

    def ready(*names):
        for name in names:
            copies[name].wait()

    seqs, _ = tokens_ref.shape
    length = kbuf.shape[1]
    rows = seqs * HEADS
    ready("tokens", "again", "wf", "fbias", "lengths")
    x = tokens_ref[...].astype(F32)
    scale = lax.rsqrt(jnp.mean(x * x, axis=1, keepdims=True) + EPS)
    normed = (x * scale * again_ref[...]).astype(BF16)
    forget = lax.dot_general(normed, wf_ref[...], NT, preferred_element_type=F32) + fbias_ref[...]
    log_forget = jax.nn.log_sigmoid(forget)
    row = lax.broadcasted_iota(jnp.int32, (rows, seqs), 0)
    col = lax.broadcasted_iota(jnp.int32, (rows, seqs), 1)
    spread_mask = (row // HEADS) == col
    spread = jnp.where(spread_mask, 1.0, 0.0).astype(BF16)
    live_len = jnp.sum(jnp.where(spread_mask, lengths_ref[...], 0), axis=1, keepdims=True)
    head8 = lax.broadcasted_iota(jnp.int32, (rows, HEADS), 0) % HEADS
    lane8 = lax.broadcasted_iota(jnp.int32, (rows, HEADS), 1)
    lf_rows = lax.dot_general(
        jnp.where(spread_mask, 1.0, 0.0), log_forget, (((1,), (0,)), ((), ())),
        precision=lax.Precision.HIGHEST, preferred_element_type=F32)
    lf_rows = jnp.sum(jnp.where(head8 == lane8, lf_rows, 0.0), axis=1, keepdims=True)

    ready("wq", "wk", "wv")
    query = dot(normed, wq[...]).astype(BF16)
    key_new = dot(normed, wk[...]).astype(BF16)
    value_new = dot(normed, wv[...]).astype(BF16)
    q_rows = dot(spread, query)
    key_rows = dot(spread, key_new)
    value_rows = dot(spread, value_new)
    head = lax.broadcasted_iota(jnp.int32, (rows, 128), 0) % HEADS
    lane = lax.broadcasted_iota(jnp.int32, (rows, 128), 1)
    half = lane // HEAD_DIM
    kv_half = head // (HEADS // KV_HEADS)
    q_sel = jnp.zeros((rows, 128), F32)
    for b in range(HEADS // 2):
        block = q_rows[:, 128 * b:128 * b + 128]
        turned = pltpu.roll(block, HEAD_DIM, 1)
        q_sel = jnp.where(head // 2 == b, jnp.where(head % 2 == kv_half, block, turned), q_sel)
    q_sel = jnp.where(half == kv_half, q_sel, 0.0)
    own = jnp.sum(q_sel * key_rows, axis=1, keepdims=True) * (HEAD_DIM ** -0.5)
    q_bf = q_sel.astype(BF16)
    seq_row = lax.broadcasted_iota(jnp.int32, (rows, 128), 0) // HEADS
    blocks = [jnp.where(seq_row == s, q_sel, 0.0).astype(BF16) for s in range(seqs)]
    q_block = jnp.concatenate(blocks, axis=1)

    ready("keys")
    k_all = jnp.concatenate([kbuf[s] for s in range(seqs)], axis=1)
    scores_t = lax.dot_general(k_all, q_block, NT, preferred_element_type=F32)
    scores = jnp.transpose(scores_t)
    ready("logcum")
    logcum = cbuf[...].reshape(rows, length)
    place = lax.broadcasted_iota(jnp.int32, (rows, length), 1)
    last = jnp.sum(jnp.where(place == live_len - 1, logcum, 0.0), axis=1, keepdims=True)
    carried = last + lf_rows
    scores = scores * (HEAD_DIM ** -0.5) + (carried - logcum)
    scores = jnp.where(place < live_len, scores, -jnp.inf)
    top = jnp.maximum(jnp.max(scores, axis=1, keepdims=True), own)
    expo = jnp.exp(scores - top)
    own_expo = jnp.exp(own - top)
    total = jnp.sum(expo, axis=1, keepdims=True) + own_expo
    weights = (expo / total).astype(BF16)
    own_weight = (own_expo / total).astype(BF16).astype(F32)

    ready("values")
    parts = []
    for p in range(seqs // 2):
        v_pair = jnp.concatenate([vbuf[2 * p], vbuf[2 * p + 1]], axis=1)
        both = dot(weights[16 * p:16 * p + 16], v_pair)
        parts.append(both[:8, :128])
        parts.append(both[8:, 128:])
    out = jnp.concatenate(parts, axis=0) + own_weight * value_rows
    out = jnp.where(half == kv_half, out, 0.0)
    out_turned = pltpu.roll(out, HEAD_DIM, 1)
    outs = []
    for b in range(HEADS // 2):
        piece = jnp.where(head // 2 == b, jnp.where(head % 2 == kv_half, out, out_turned), 0.0)
        outs.append(lax.dot_general(spread, piece.astype(BF16), TN, preferred_element_type=F32))
    attended = jnp.concatenate(outs, axis=1).astype(BF16)
    ready("wo", "egain", "bgate", "ids", "eweights")
    mixed = (x + dot(attended, wo[...])).astype(BF16)
    mixed_ref[...] = mixed
    y = mixed.astype(F32)
    scale = lax.rsqrt(jnp.mean(y * y, axis=1, keepdims=True) + EPS)
    routed_in = (y * scale * egain_ref[...]).astype(BF16)
    branch = jax.nn.sigmoid(jnp.sum(routed_in.astype(F32) * bgate_ref[...], axis=1, keepdims=True))
    branch_ref[...] = jnp.broadcast_to(branch, branch_ref.shape)
    routed_ref[...] = routed_in
    fill_outgoing(routed_in, ids_ref, eweights_ref, place_ref, outgoing_ref)


def mixer(tokens, attn_norm_gain, w_query, w_key, w_value, w_forget, forget_bias, w_attn_out,
          cache_keys, cache_values, cache_logcum, cache_lengths, expert_norm_gain, branch_gate,
          expert_ids, expert_weights, devices):
    seqs, width = tokens.shape
    operands = (
        tokens, attn_norm_gain.reshape(1, width), w_query, w_key, w_value, w_forget.T,
        forget_bias.reshape(1, HEADS), w_attn_out, cache_keys, cache_values, cache_logcum,
        cache_lengths.reshape(1, seqs), expert_norm_gain.reshape(1, width),
        branch_gate.reshape(1, width), expert_ids.T, expert_weights.T)
    operands = tuple(pltpu.with_memory_space_constraint(a, pltpu.HBM) for a in operands)
    return pl.pallas_call(
        mixer_body,
        out_shape=(
            jax.ShapeDtypeStruct((seqs, width), BF16),
            jax.ShapeDtypeStruct((seqs, width), BF16),
            jax.ShapeDtypeStruct((seqs, 128), F32),
            jax.ShapeDtypeStruct((devices * CAP, seqs), F32),
            jax.ShapeDtypeStruct((devices, CAP, width), BF16),
        ),
        in_specs=[HBM] * len(operands),
        out_specs=(VMEM,) * 5,
        scratch_shapes=[pltpu.VMEM(a.shape, a.dtype) for a in operands]
        + [pltpu.SemaphoreType.DMA((len(operands),))],
        compiler_params=pltpu.CompilerParams(vmem_limit_bytes=28 * 1024 * 1024),
        cost_estimate=pl.CostEstimate(flops=10**10, bytes_accessed=15 * 2**20, transcendentals=0),
        name="mixer",
    )(*operands)


def worker_body(arrived_ref, gate_hbm, up_hbm, down_hbm, answer_ref, wg, wu, wd, sems):
    devices, cap, width = arrived_ref.shape
    rows = devices * cap
    copies = [
        pltpu.make_async_copy(source.at[0], target, sems.at[i])
        for i, (source, target) in enumerate(((gate_hbm, wg), (up_hbm, wu), (down_hbm, wd)))]
    for copy in copies:
        copy.start()
    x = arrived_ref[...].reshape(rows, width)
    copies[0].wait()
    gate = jnp.minimum(dot(x, wg[...]), LIMIT)
    copies[1].wait()
    up = jnp.clip(dot(x, wu[...]), -LIMIT, LIMIT)
    act = ((up + 1.0) * gate * jax.nn.sigmoid(gate * ALPHA)).astype(BF16)
    copies[2].wait()
    answer_ref[...] = dot(act, wd[...]).astype(BF16).reshape(devices, cap, width)


def worker(arrived, gate_w, up_w, down_w):
    stored = tuple(
        pltpu.with_memory_space_constraint(a, pltpu.HBM) for a in (gate_w, up_w, down_w))
    return pl.pallas_call(
        worker_body,
        out_shape=jax.ShapeDtypeStruct(arrived.shape, BF16),
        in_specs=[VMEM] + [HBM] * 3,
        out_specs=VMEM,
        scratch_shapes=[pltpu.VMEM(a.shape[1:], BF16) for a in stored]
        + [pltpu.SemaphoreType.DMA((3,))],
        compiler_params=pltpu.CompilerParams(vmem_limit_bytes=20 * 1024 * 1024),
        cost_estimate=pl.CostEstimate(flops=3 * 10**9, bytes_accessed=8 * 2**20, transcendentals=0),
        name="worker",
    )(arrived, *stored)


def two_parts(square, rows):
    lane = lax.broadcasted_iota(jnp.int32, (rows, 128), 1)
    top = square.astype(BF16).astype(F32)
    return jnp.where(lane == 0, top, jnp.where(lane == 1, square - top, 0.0))


def dense_body(
    device_ref, rows_ref, h0, h1, h2, h3, h4, h5, h6, h7, gain_ref,
    o0, o1, o2, o3, held, sems,
):
    rows, width = rows_ref.shape
    devices = PLANE * SIDE
    copies = [
        pltpu.make_async_copy(source, held.at[i], sems.at[i])
        for i, source in enumerate((h0, h1, h2, h3, h4, h5, h6, h7))]
    for copy in copies:
        copy.start()
    units = held.shape[1] // 3
    me = device_ref[0]
    gains = []
    lane = lax.broadcasted_iota(jnp.int32, (1, 128), 1)
    per_row = 128 // units
    for block in range(PARTS // per_row):
        vec = jnp.zeros((1, 128), F32)
        for q in range(per_row):
            p = block * per_row + q
            owner = lax.rem(me + (SIDE - p // CORES) * PLANE, devices)
            if p % CORES:
                owner = owner + 1 - 2 * lax.rem(me, CORES)
            line = gain_ref[pl.ds(owner // per_row, 1), :]
            shift = lax.rem(q - lax.rem(owner, per_row) + per_row, per_row) * units
            vec = jnp.where(lane // units == q, pltpu.roll(line, shift, 1), vec)
        gains.append(vec)
    gain = jnp.concatenate(gains, axis=1)
    for copy in copies:
        copy.wait()
    dg = jnp.concatenate([held[p, :units] for p in range(PARTS)], axis=0)
    du = jnp.concatenate([held[p, units:2 * units] for p in range(PARTS)], axis=0)
    dd = jnp.concatenate([held[p, 2 * units:] for p in range(PARTS)], axis=0)
    x = rows_ref[...]
    gate = lax.dot_general(x, dg, NT, preferred_element_type=F32)
    up = lax.dot_general(x, du, NT, preferred_element_type=F32)
    kept = (jax.nn.silu(gate) * up).astype(BF16).astype(F32)
    square = jnp.sum(kept * kept, axis=1, keepdims=True)
    total = dot((kept * gain).astype(BF16), dd)
    parts = two_parts(square, rows)
    step = rows // SIDE
    for k, out in enumerate((o0, o1, o2, o3)):
        out[:, :width] = total[k * step:(k + 1) * step].astype(BF16)
        out[:, width:] = parts[k * step:(k + 1) * step].astype(BF16)


def dense_units(device, rows, pieces, gain):
    pieces = tuple(pltpu.with_memory_space_constraint(a, pltpu.HBM) for a in pieces)
    count, width = rows.shape
    return pl.pallas_call(
        dense_body,
        out_shape=tuple(
            jax.ShapeDtypeStruct((count // SIDE, width + 128), BF16) for _ in range(SIDE)),
        in_specs=[pl.BlockSpec(memory_space=pltpu.SMEM), VMEM] + [HBM] * len(pieces) + [VMEM],
        out_specs=(VMEM,) * SIDE,
        scratch_shapes=[
            pltpu.VMEM((len(pieces),) + pieces[0].shape, BF16),
            pltpu.SemaphoreType.DMA((len(pieces),)),
        ],
        compiler_params=pltpu.CompilerParams(vmem_limit_bytes=20 * 1024 * 1024),
        cost_estimate=pl.CostEstimate(flops=2 * 10**9, bytes_accessed=6 * 2**20, transcendentals=0),
        name="dense",
    )(device, rows, *pieces, gain.reshape(-1, 128))


def fold_body(a, b, c, d, o0, o1, o2, o3):
    rows = a.shape[0]
    width = a.shape[1] - 128
    total = sum(r[:, :width].astype(F32) for r in (a, b, c, d))
    squares = sum(r[:, width:].astype(F32) for r in (a, b, c, d))
    parts = two_parts(jnp.sum(squares, axis=1, keepdims=True), rows)
    step = rows // SIDE
    for k, out in enumerate((o0, o1, o2, o3)):
        out[:, :width] = total[k * step:(k + 1) * step].astype(BF16)
        out[:, width:] = parts[k * step:(k + 1) * step].astype(BF16)


def fold(blocks):
    rows, packed = blocks[0].shape
    return pl.pallas_call(
        fold_body,
        out_shape=tuple(jax.ShapeDtypeStruct((rows // SIDE, packed), BF16) for _ in range(SIDE)),
        in_specs=[VMEM] * SIDE,
        out_specs=(VMEM,) * SIDE,
        compiler_params=pltpu.CompilerParams(vmem_limit_bytes=12 * 1024 * 1024),
        name="fold",
    )(*blocks)


def merger_body(returned_ref, place_ref, mixed_ref, branch_ref, a, b, c, d, result_ref):
    devices, cap, width = returned_ref.shape
    rows = devices * cap
    total = sum(r[:, :width].astype(F32) for r in (a, b, c, d))
    squares = sum(r[:, width:].astype(F32) for r in (a, b, c, d))
    unit_scale = lax.rsqrt(jnp.sum(squares, axis=1, keepdims=True) / DENSE_FF + EPS)
    base = mixed_ref[...].astype(F32) + branch_ref[:, :1] * (total * unit_scale)

    def tn(a, b):
        return lax.dot_general(a, b, TN, preferred_element_type=F32)

    share = place_ref[...]
    s1 = share.astype(BF16)
    rest = share - s1.astype(F32)
    s2 = rest.astype(BF16)
    s3 = (rest - s2.astype(F32)).astype(BF16)
    answers = returned_ref[...].reshape(rows, width)
    routed = tn(s1, answers) + tn(s2, answers) + tn(s3, answers)
    result_ref[...] = (base + routed).astype(BF16)


def merger(returned, place, mixed, branch, blocks):
    return pl.pallas_call(
        merger_body,
        out_shape=jax.ShapeDtypeStruct(mixed.shape, BF16),
        in_specs=[VMEM] * (4 + SIDE),
        out_specs=VMEM,
        compiler_params=pltpu.CompilerParams(vmem_limit_bytes=16 * 1024 * 1024),
        name="merger",
    )(returned, place, mixed, branch, *blocks)


def shifted(array, devices, stride, by):
    ring = stride * SIDE
    pairs = [
        (d, d // ring * ring + (d % ring + by * stride) % ring) for d in range(devices)]
    return lax.ppermute(array, "ep", pairs)


def exchange(blocks, devices, stride, sign):
    out = [blocks[0]]
    for k in range(1, SIDE):
        out.append(shifted(blocks[k], devices, stride, sign * k))
    return out


def gather_pieces(own, devices):
    def moved(array, target):
        return lax.ppermute(array, "ep", [(d, target(d)) for d in range(devices)])

    pieces = []
    for hop in range(PARTS // CORES):
        mine = own
        if hop:
            mine = moved(own, lambda d: (d + hop * PLANE) % devices)
        pieces.append(mine)
        pieces.append(moved(mine, lambda d: d ^ 1))
    return pieces


def layer(
    tokens, attn_norm_gain, w_query, w_key, w_value, w_forget, forget_bias, w_attn_out,
    cache_keys, cache_values, cache_logcum, cache_lengths, expert_norm_gain, expert_ids,
    expert_weights, w_expert_gate, w_expert_up, w_expert_down, w_dense_gate, w_dense_up,
    w_dense_down, dense_norm_gain, branch_gate,
):
    devices = lax.axis_size("ep")
    across, along = CORES, CORES * SIDE
    me = lax.axis_index("ep").astype(jnp.int32).reshape(1)
    own = jnp.concatenate([w_dense_gate.T, w_dense_up.T, w_dense_down], axis=0)
    pieces = gather_pieces(own, devices)
    mixed, routed_in, branch, place, outgoing = mixer(
        tokens, attn_norm_gain, w_query, w_key, w_value, w_forget, forget_bias, w_attn_out,
        cache_keys, cache_values, cache_logcum, cache_lengths, expert_norm_gain, branch_gate,
        expert_ids, expert_weights, devices)
    arrived = lax.all_to_all(outgoing, "ep", split_axis=0, concat_axis=0, tiled=True)
    row = jnp.concatenate(exchange([routed_in] * SIDE, devices, across, 1), axis=0)
    rows = jnp.concatenate(exchange([row] * SIDE, devices, along, 1), axis=0)
    partial = dense_units(me, rows, pieces, dense_norm_gain)
    partial = exchange(partial, devices, along, -1)
    partial = fold(partial)
    partial = exchange(partial, devices, across, -1)
    answer = worker(arrived, w_expert_gate, w_expert_up, w_expert_down)
    returned = lax.all_to_all(answer, "ep", split_axis=0, concat_axis=0, tiled=True)
    return merger(returned, place, mixed, branch, partial)


def solution(mesh):
    in_specs = (
        P("ep", None),
        P(),
        P(),
        P(),
        P(),
        P(),
        P(),
        P(),
        P("ep", None, None),
        P("ep", None, None),
        P("ep", None, None),
        P("ep"),
        P(),
        P("ep", None),
        P("ep", None),
        P("ep", None, None),
        P("ep", None, None),
        P("ep", None, None),
        P(None, "ep"),
        P(None, "ep"),
        P("ep", None),
        P(),
        P(),
    )
    out_specs = P("ep", None)
    return jax.shard_map(
        layer, mesh=mesh, in_specs=in_specs, out_specs=out_specs, check_vma=False)
```
